32 devices in a mesh: dp: 4 (over y, x), kv: 4 (over z), tp: 2 (over core).
Axes of the slice: x: 2, y: 2, z: 4, core: 2. Of those that a mesh axis runs over, the one named last changes fastest.
Arguments:
- tokens: bfloat16 [4, 3072, 2048], P('dp', 'kv'), may hold values from -60 to 60
- query_weight: bfloat16 [2048, 1024], P(None, 'tp'), may hold values from -0.125 to 0.125
- key_weight: bfloat16 [2048, 256], P(None, 'tp'), may hold values from -0.125 to 0.125
- value_weight: bfloat16 [2048, 256], P(None, 'tp'), may hold values from -0.125 to 0.125
- out_weight: bfloat16 [1024, 2048], P('tp'), may hold values from -3 to 3
- norm_gain: float32 [2048], P('tp'), may hold values from 0.1 to 1.9
- chosen_owner: int32 [4, 24, 4], P('dp'), may hold values from -1 to 3, as said below
- chosen_part: int32 [4, 24, 4], P('dp'), may hold values from 0 to 11, as said below
Outputs:
- attended: bfloat16 [4, 3072, 2048], P('dp', 'kv', 'tp')
The draws below stay inside these ranges and needn't reach their ends.
Inputs may be any that keep to these rules, and one draw needn't show every extreme that they name: `chosen_owner`: within a row the indices other than -1 are different. Every named key block lies wholly before its query block's first position. Among the 6 rows of one index of kv, no index is named by more than 6 rows. `chosen_part`: 0 where the owner is -1.
All inputs are finite; a program needn't handle non-finite values.
Results may differ from the reference program's by a relative error of at most 0.014.
The reference program's roundings to bfloat16 on the way count: a program that leaves them out, or rounds other values in their place, can miss the bound.
Values may be sent and summed in bfloat16 or wider, within the bound.
No kernel may reach another device: no remote copies, remote signals or barrier semaphores. Data moves between devices by JAX's collectives and lax.ppermute only.
A program may use at most 128 MiB of HBM per device.

```python
import jax
import jax.numpy as jnp
from jax import lax

D = 2048
HEADS = 16
KV_HEADS = 4
HEAD_DIM = 64
QUERY_BLOCK = 128
KEY_BLOCK = 64
SEQS = 4
SEQ = 3072
QBLOCKS = 24
QBLOCKS_DEV = 6
KBLOCKS_DEV = 12
CHOSEN = 4
N_KV = 4
N_TP = 2


def draw_tokens(key, part):
    base = jax.random.normal(jax.random.fold_in(key, 11), (SEQS, SEQ, D), jnp.float32)
    base = jnp.clip(base, -6.0, 6.0)
    return base.astype(jnp.bfloat16)


def draw_out_weight(key, part):
    base = jax.random.normal(jax.random.fold_in(key, 21), (HEADS * HEAD_DIM, D), jnp.float32)
    base = jnp.clip(base, -6.0, 6.0) * (HEADS * HEAD_DIM) ** (-0.5)
    column = jnp.arange(D, dtype=jnp.float32) / D
    jitter = jnp.exp(jax.random.uniform(jax.random.fold_in(key, 22), (D,), jnp.float32, -0.5, 0.5))
    rising = 3.0 ** column
    return (base * (rising * jitter)[None, :] * 0.5).astype(jnp.bfloat16)


def chosen_pair(key):
    block_ids = jnp.arange(QBLOCKS, dtype=jnp.int32)
    device_ids = block_ids // QBLOCKS_DEV
    local_ids = block_ids % QBLOCKS_DEV
    owners = jnp.arange(N_KV, dtype=jnp.int32)
    earlier = owners[None, :] < device_ids[:, None]
    itself = jnp.logical_and(owners[None, :] == device_ids[:, None], local_ids[:, None] > 0)
    allowed = jnp.logical_or(earlier, itself)
    forced = jnp.logical_or(jnp.logical_or(owners[None, :] == 0, owners[None, :] == device_ids[:, None] - 1), jnp.logical_or(owners[None, :] == device_ids[:, None] - N_KV // 2, owners[None, :] == device_ids[:, None]))
    forced = jnp.logical_and(forced, allowed)
    noise = jax.random.randint(jax.random.fold_in(key, 31), (SEQS, QBLOCKS, N_KV), 0, 16384)
    scores = noise + (N_KV - owners)[None, None, :] * (16384 // N_KV) + forced[None].astype(jnp.int32) * 1048576
    scores = jnp.where(allowed[None], scores, -2097152)
    scores = scores * 64 + owners[None, None, :]
    picked = lax.top_k(scores, CHOSEN)[1].astype(jnp.int32)
    valid = jnp.take_along_axis(jnp.broadcast_to(allowed[None], (SEQS, QBLOCKS, N_KV)), picked, axis=2)
    owner_out = jnp.where(valid, picked, -1).astype(jnp.int32)
    limit = jnp.where(picked == device_ids[None, :, None], QUERY_BLOCK // KEY_BLOCK * local_ids[None, :, None], KBLOCKS_DEV)
    limit = jnp.maximum(limit, 1)
    raw_part = jax.random.randint(jax.random.fold_in(key, 32), (SEQS, QBLOCKS, CHOSEN), 0, 1048576)
    part_out = jnp.where(valid, raw_part % limit, 0).astype(jnp.int32)
    return (owner_out, part_out)


def draw_chosen_owner(key, part):
    return chosen_pair(jax.random.fold_in(key, 41))[0]


def draw_chosen_part(key, part):
    return chosen_pair(jax.random.fold_in(key, 41))[1]


def level_of(own_key, dims, cuts, least, high):
    gain, own = 1.0, jax.random.fold_in(own_key, 6)
    for axis_at, parts in cuts:
        draws = jnp.exp(jax.random.uniform(jax.random.fold_in(own, axis_at), (parts,), jnp.float32, least / len(cuts), high / len(cuts)))
        gain = gain * jnp.repeat(draws, dims[axis_at] // parts).reshape([-1 if axis == axis_at else 1 for axis in range(len(dims))])
    return gain


def bell_draw(rng, shape, deviation, bound, split=(), held_as=jnp.bfloat16):
    factor_of = level_of(rng, shape, split, -0.22, 0.18) if split else 1.0
    drawn = jax.random.normal(rng, shape, jnp.float32) * deviation * factor_of
    return jnp.minimum(jnp.maximum(drawn, -bound), bound).astype(held_as)


def setup_inputs(seed: int = 0) -> dict:
    keys = jax.random.split(jax.random.key(seed), 9)
    tokens = draw_tokens(jax.random.fold_in(keys[8], 71), 0)
    query_weight = bell_draw(keys[1], (D, HEADS * HEAD_DIM), D ** -0.5, 0.125, ((1, 2),))
    key_weight = bell_draw(keys[2], (D, KV_HEADS * HEAD_DIM), D ** -0.5, 0.125, ((1, 2),))
    value_weight = bell_draw(keys[3], (D, KV_HEADS * HEAD_DIM), D ** -0.5, 0.125, ((1, 2),))
    out_weight = draw_out_weight(jax.random.fold_in(keys[8], 71), 0)
    norm_gain = jnp.clip(1.0 + 0.18 * jax.random.normal(keys[5], (D,), jnp.float32), 0.1, 1.9)
    chosen_owner = draw_chosen_owner(jax.random.fold_in(keys[8], 71), 0)
    chosen_part = draw_chosen_part(jax.random.fold_in(keys[8], 71), 0)
    return {"tokens": tokens, "query_weight": query_weight, "key_weight": key_weight, "value_weight": value_weight, "out_weight": out_weight, "norm_gain": norm_gain, "chosen_owner": chosen_owner, "chosen_part": chosen_part}


rope_base = 10000.0
norm_eps = 1e-06

def rotate(head_rows, positions):
    half_dim = head_rows.shape[-1] // 2
    frequency = rope_base ** (-jnp.arange(half_dim, dtype=jnp.float32) / half_dim)
    angles = positions.astype(jnp.float32)[:, None] * frequency
    cosine = jnp.cos(angles)[:, None, :]
    sine_part = jnp.sin(angles)[:, None, :]
    first_half = head_rows[..., :half_dim]
    second_half = head_rows[..., half_dim:]
    return jnp.concatenate([first_half * cosine - second_half * sine_part, second_half * cosine + first_half * sine_part], axis=-1)

def reference(tokens, query_weight, key_weight, value_weight, out_weight, norm_gain, chosen_owner, chosen_part):
    group_size = HEADS // KV_HEADS
    lower_mask = jnp.arange(QUERY_BLOCK)[:, None] >= jnp.arange(QUERY_BLOCK)[None, :]

    def one_sequence(seq_items):
        row_data, owner_ids, part_ids = seq_items
        positions = jnp.arange(SEQ, dtype=jnp.int32)
        queries = rotate(jnp.dot(row_data, query_weight, preferred_element_type=jnp.float32).reshape(SEQ, HEADS, HEAD_DIM), positions).astype(jnp.bfloat16)
        key_rows = rotate(jnp.dot(row_data, key_weight, preferred_element_type=jnp.float32).reshape(SEQ, KV_HEADS, HEAD_DIM), positions).astype(jnp.bfloat16)
        value_rows = jnp.dot(row_data, value_weight, preferred_element_type=jnp.float32).astype(jnp.bfloat16).reshape(SEQ, KV_HEADS, HEAD_DIM)
        key_blocks = key_rows.reshape(SEQ // KEY_BLOCK, KEY_BLOCK, KV_HEADS, HEAD_DIM)
        value_blocks = value_rows.reshape(SEQ // KEY_BLOCK, KEY_BLOCK, KV_HEADS, HEAD_DIM)
        slot_valid = owner_ids >= 0
        chosen_ids = jnp.where(slot_valid, owner_ids * KBLOCKS_DEV + part_ids, 0).astype(jnp.int32)

        def one_block(block_index):
            block_start = (block_index * QUERY_BLOCK).astype(jnp.int32)
            picked_ids = chosen_ids[block_index]
            valid_row = slot_valid[block_index]
            block_queries = lax.dynamic_slice_in_dim(queries, block_start, QUERY_BLOCK, 0).reshape(QUERY_BLOCK, KV_HEADS, group_size, HEAD_DIM).astype(jnp.float32)
            own_keys = lax.dynamic_slice_in_dim(key_rows, block_start, QUERY_BLOCK, 0)
            own_values = lax.dynamic_slice_in_dim(value_rows, block_start, QUERY_BLOCK, 0)
            chosen_keys = key_blocks[picked_ids].reshape(CHOSEN * KEY_BLOCK, KV_HEADS, HEAD_DIM)
            chosen_values = value_blocks[picked_ids].reshape(CHOSEN * KEY_BLOCK, KV_HEADS, HEAD_DIM)
            all_keys = jnp.concatenate([chosen_keys, own_keys], axis=0).astype(jnp.float32)
            all_values = jnp.concatenate([chosen_values, own_values], axis=0).astype(jnp.float32)
            key_valid = jnp.broadcast_to(valid_row[:, None], (CHOSEN, KEY_BLOCK)).reshape(CHOSEN * KEY_BLOCK)
            far_mask = jnp.broadcast_to(key_valid[None, :], (QUERY_BLOCK, CHOSEN * KEY_BLOCK))
            full_mask = jnp.concatenate([far_mask, lower_mask], axis=1)
            scores = jnp.einsum('qngd,knd->ngqk', block_queries, all_keys) * HEAD_DIM ** (-0.5)
            scores = jnp.where(full_mask[None, None], scores, -jnp.inf)
            row_max = lax.optimization_barrier(jnp.max(scores, axis=-1, keepdims=True))
            weights = jnp.exp(scores - row_max)
            weights = (weights / lax.optimization_barrier(jnp.sum(weights, axis=-1, keepdims=True))).astype(jnp.bfloat16)
            mixed_out = jnp.einsum('ngqk,knd->qngd', weights.astype(jnp.float32), all_values)
            return mixed_out.reshape(QUERY_BLOCK, HEADS * HEAD_DIM).astype(jnp.bfloat16)
        mixed_rows = lax.map(one_block, jnp.arange(QBLOCKS, dtype=jnp.int32)).reshape(SEQ, HEADS * HEAD_DIM)
        share_cols = HEADS * HEAD_DIM // N_TP
        summed = jnp.zeros((SEQ, D), jnp.float32)
        for member in range(N_TP):
            partial_value = jnp.dot(mixed_rows[:, member * share_cols:(member + 1) * share_cols], out_weight[member * share_cols:(member + 1) * share_cols], preferred_element_type=jnp.float32).astype(jnp.bfloat16)
            summed = summed + lax.optimization_barrier(partial_value).astype(jnp.float32)
        mean_sq = lax.optimization_barrier(jnp.mean(summed * summed, axis=1, keepdims=True))
        return (summed * lax.rsqrt(mean_sq + norm_eps) * norm_gain.astype(jnp.float32)).astype(jnp.bfloat16)
    return lax.map(one_sequence, (tokens, chosen_owner, chosen_part))
```

```python
import functools

import jax
import jax.numpy as jnp
import numpy as np
from jax import lax
from jax.experimental import pallas as pl
from jax.experimental.pallas import tpu as pltpu
from jax.sharding import PartitionSpec as P

HEAD_DIM = 64
QUERY_BLOCK = 128
KEY_BLOCK = 64
LANES = 128
ROPE_BASE = 10000.0
NORM_EPS = 1e-06
LOG2E = 1.4426950408889634
GROUPS = 1

BF16 = jnp.bfloat16
F32 = jnp.float32
HBM = pltpu.MemorySpace.HBM
SMEM = pltpu.MemorySpace.SMEM
VMEM = pltpu.MemorySpace.VMEM


def angle_tables(length):
    half = HEAD_DIM // 2
    frequency = ROPE_BASE ** (-np.arange(half, dtype=np.float64) / half)
    lane_frequency = np.tile(frequency, LANES // half)
    sign = np.tile(np.repeat([-1.0, 1.0], half), LANES // HEAD_DIM)
    coarse = (np.arange(length // KEY_BLOCK) * KEY_BLOCK)[:, None] * lane_frequency
    fine = np.arange(KEY_BLOCK)[:, None] * lane_frequency
    make = lambda a: np.stack([np.cos(a), np.sin(a) * sign], 1).astype(np.float32)
    return make(coarse), np.swapaxes(make(fine), 0, 1).copy()


def rotate_tile(tile, cosine, sine):
    lane = lax.broadcasted_iota(jnp.int32, tile.shape, 1)
    half = HEAD_DIM // 2
    first = (lane % HEAD_DIM) < half
    swapped = jnp.where(
        first, pltpu.roll(tile, LANES - half, 1), pltpu.roll(tile, half, 1)
    )
    return tile * cosine + swapped * sine


def block_angles(coarse_ref, fine_ref, block):
    coarse = coarse_ref[block]
    c_a, s_a = coarse[0:1], coarse[1:2]
    c_b, s_b = fine_ref[0], fine_ref[1]
    return c_a * c_b - s_a * s_b, s_a * c_b + c_a * s_b


def wanted_block(owner_ref, part_ref, row, me):
    total = jnp.int32(0)
    for slot in range(owner_ref.shape[0]):
        total = total + jnp.where(owner_ref[slot, row] == me, part_ref[slot, row], 0)
    return total


def kv_kernel(plan, devices, chunk, *refs):
    (owner_ref, part_ref, tokens_ref, wk_ref, wv_ref, coarse_ref, fine_ref), refs = refs[:7], refs[7:]
    kv_ref, refs = refs[0], refs[1:]
    send_refs, (tok, weight, tok_sem, w_sem) = refs[: len(plan)], refs[len(plan) :]
    rows = tok.shape[0]
    me = lax.axis_index("kv")
    w_copies = [
        pltpu.make_async_copy(src, weight.at[:, pl.ds(at * LANES, LANES)], w_sem.at[at])
        for at, src in enumerate((wk_ref, wv_ref))
    ]
    t_copies = [
        pltpu.make_async_copy(
            tokens_ref.at[0, pl.ds(at * chunk, chunk)], tok.at[pl.ds(at * chunk, chunk)], tok_sem.at[at]
        )
        for at in range(rows // chunk)
    ]
    for copy in w_copies + t_copies:
        copy.start()
    for copy in w_copies:
        copy.wait()
    per_chunk = chunk // KEY_BLOCK
    blocks = rows // KEY_BLOCK
    for at in range(rows // chunk):
        t_copies[at].wait()
        product = jnp.dot(
            tok[pl.ds(at * chunk, chunk)], weight[...], preferred_element_type=F32
        )
        for sub in range(per_chunk):
            block = at * per_chunk + sub
            cosine, sine = block_angles(coarse_ref, fine_ref, me * blocks + block)
            piece = product[sub * KEY_BLOCK : (sub + 1) * KEY_BLOCK]
            kv_ref[block, :, 0:LANES] = rotate_tile(piece[:, :LANES], cosine, sine).astype(BF16)
            kv_ref[block, :, LANES : 2 * LANES] = piece[:, LANES:].astype(BF16)
    qblocks = rows // QUERY_BLOCK
    for (kind, arg, first), out in zip(plan, send_refs):
        if kind == "shift":
            target = jnp.minimum(me + arg, devices - 1)
            for row in range(out.shape[0]):
                out[row] = kv_ref[wanted_block(owner_ref, part_ref, target * qblocks + first + row, me)]
        else:
            def fill(index, carry, out=out):
                out[index] = kv_ref[wanted_block(owner_ref, part_ref, index, me)]
                return carry
            lax.fori_loop(0, out.shape[0], fill, 0)


def q_kernel(tokens_ref, wq_ref, coarse_ref, fine_ref, out_ref):
    rows = tokens_ref.shape[1]
    step = pl.program_id(0)
    total_blocks = pl.num_programs(0) * (rows // KEY_BLOCK)
    me = lax.axis_index("kv")
    product = jnp.dot(tokens_ref[0], wq_ref[...], preferred_element_type=F32) * (HEAD_DIM ** -0.5)
    tiles = product.shape[1] // LANES
    lane = lax.broadcasted_iota(jnp.int32, (KEY_BLOCK, LANES), 1)
    low = lane < HEAD_DIM
    for sub in range(rows // KEY_BLOCK):
        cosine, sine = block_angles(
            coarse_ref, fine_ref, me * total_blocks + step * (rows // KEY_BLOCK) + sub
        )
        span = slice(sub * KEY_BLOCK, (sub + 1) * KEY_BLOCK)
        for tile in range(tiles):
            piece = rotate_tile(product[span, tile * LANES : (tile + 1) * LANES], cosine, sine)
            other = pltpu.roll(piece, HEAD_DIM, 1)
            if tile < tiles // 2:
                even, odd = jnp.where(low, piece, 0.0), jnp.where(low, other, 0.0)
            else:
                even, odd = jnp.where(low, 0.0, other), jnp.where(low, 0.0, piece)
            out_ref[span, (2 * tile) * LANES : (2 * tile + 1) * LANES] = even.astype(BF16)
            out_ref[span, (2 * tile + 1) * LANES : (2 * tile + 2) * LANES] = odd.astype(BF16)


def attention_kernel(sources, valid_ref, q_ref, own_ref, *refs):
    source_refs, out_ref = refs[:sources], refs[sources]
    step = pl.program_id(0)
    heads = q_ref.shape[1] // LANES
    pairs = heads // 2
    own = own_ref[...].reshape(QUERY_BLOCK, 2 * LANES)
    picks = [ref[0] for ref in source_refs]
    keys = jnp.concatenate([p[:, :LANES] for p in picks] + [own[:, :LANES]], axis=0)
    values = jnp.concatenate([p[:, LANES:] for p in picks] + [own[:, LANES:]], axis=0)
    values = jnp.concatenate([values, jnp.ones_like(values)], axis=1)
    far = sources * KEY_BLOCK
    lane = lax.broadcasted_iota(jnp.int32, (1, far), 1)
    bias = jnp.zeros((1, far), F32)
    for at in range(sources):
        level = jnp.where(valid_ref[step, at] > 0, jnp.float32(0), jnp.float32(-jnp.inf))
        bias = jnp.where(lane // KEY_BLOCK == at, level, bias)
    row_id = lax.broadcasted_iota(jnp.int32, (2 * QUERY_BLOCK, QUERY_BLOCK), 0) % QUERY_BLOCK
    col_id = lax.broadcasted_iota(jnp.int32, (2 * QUERY_BLOCK, QUERY_BLOCK), 1)
    lower = row_id >= col_id
    low = lax.broadcasted_iota(jnp.int32, (QUERY_BLOCK, LANES), 1) < HEAD_DIM
    for pair in range(pairs):
        query = jnp.concatenate(
            [q_ref[:, h * LANES : (h + 1) * LANES] for h in (pair, pair + pairs)], axis=0
        )
        scores = lax.dot_general(
            query, keys, (((1,), (1,)), ((), ())), preferred_element_type=F32
        )
        scores = jnp.concatenate(
            [scores[:, :far] + bias, jnp.where(lower, scores[:, far:], -jnp.inf)], axis=1
        )
        row_max = jnp.max(scores, axis=1, keepdims=True)
        weights = jnp.exp2((scores - row_max) * LOG2E).astype(BF16)
        mixed = jnp.dot(weights, values, preferred_element_type=F32)
        top = jnp.where(low, mixed[:QUERY_BLOCK, :LANES], mixed[QUERY_BLOCK:, :LANES])
        bottom = jnp.where(low, mixed[:QUERY_BLOCK, LANES:], mixed[QUERY_BLOCK:, LANES:])
        out_ref[:, pair * LANES : (pair + 1) * LANES] = (top / bottom).astype(BF16)


def out_kernel(mine_ref, other_ref, w_mine_ref, w_other_ref, gain_ref, out_ref, weight, sem):
    cols = out_ref.shape[1]
    depth = w_mine_ref.shape[0]
    heads = depth // HEAD_DIM
    copies = []
    for side, src in enumerate((w_mine_ref, w_other_ref)):
        for slot in range(heads):
            head = slot // 2 + (slot % 2) * (heads // 2)
            copies.append(
                pltpu.make_async_copy(
                    src.at[pl.ds(head * HEAD_DIM, HEAD_DIM)],
                    weight.at[side, pl.ds(slot * HEAD_DIM, HEAD_DIM)],
                    sem.at[side, slot],
                )
            )

    @pl.when(pl.program_id(0) == 0)
    def _():
        for copy in copies:
            copy.start()
        for copy in copies:
            copy.wait()

    mine, other = mine_ref[...], other_ref[...]
    me = lax.axis_index("tp")
    total = None
    width = 512
    kept = []
    for half in range(2):
        for at in range(cols // width):
            start = pl.multiple_of((me if half == 0 else 1 - me) * cols + at * width, width)
            a = jnp.dot(mine, weight[0, :, pl.ds(start, width)], preferred_element_type=F32)
            b = jnp.dot(other, weight[1, :, pl.ds(start, width)], preferred_element_type=F32)
            projected = a.astype(BF16).astype(F32) + b.astype(BF16).astype(F32)
            if half == 0:
                kept.append(projected)
            squares = jnp.sum(projected * projected, axis=1, keepdims=True)
            total = squares if total is None else total + squares
    scale = lax.rsqrt(total / (2 * cols) + NORM_EPS)
    for at, projected in enumerate(kept):
        span = slice(at * width, (at + 1) * width)
        out_ref[:, span] = (projected * scale * gain_ref[:, span]).astype(BF16)


def body(
    tokens, query_weight, key_weight, value_weight, out_weight, norm_gain, chosen_owner, chosen_part
):
    tok_count, width = tokens.shape[1], tokens.shape[2]
    devices = lax.axis_size("kv")
    me = lax.axis_index("kv")
    heads = query_weight.shape[1] // HEAD_DIM
    assert key_weight.shape[1] == LANES and value_weight.shape[1] == LANES
    per_device = tok_count // KEY_BLOCK
    qblocks = tok_count // QUERY_BLOCK
    owner_t, part_t = chosen_owner[0].T, chosen_part[0].T
    chosen = owner_t.shape[0]
    coarse, fine = (jnp.asarray(t) for t in angle_tables(devices * tok_count))
    swap = [(0, 1), (1, 0)]
    vm = pl.BlockSpec(memory_space=VMEM)
    sm = pl.BlockSpec(memory_space=SMEM)
    hb = pl.BlockSpec(memory_space=HBM)

    groups = GROUPS if qblocks % GROUPS == 0 else 1
    per_group = qblocks // groups
    direct = devices <= chosen
    plan = (
        [("shift", shift, g * per_group) for shift in range(devices) for g in range(groups)]
        if direct
        else [("all", 0, 0)]
    )
    sends = [
        jax.ShapeDtypeStruct(
            (per_group if direct else devices * qblocks, KEY_BLOCK, 2 * LANES), BF16
        )
        for _ in plan
    ]
    chunk = 256
    kv_out = pl.pallas_call(
        functools.partial(kv_kernel, plan, devices, chunk),
        out_shape=[jax.ShapeDtypeStruct((per_device, KEY_BLOCK, 2 * LANES), BF16)] + sends,
        in_specs=[sm, sm, hb, hb, hb, vm, vm],
        out_specs=[vm] * (1 + len(sends)),
        scratch_shapes=[
            pltpu.VMEM((tok_count, width), BF16),
            pltpu.VMEM((width, 2 * LANES), BF16),
            pltpu.SemaphoreType.DMA((tok_count // chunk,)),
            pltpu.SemaphoreType.DMA((2,)),
        ],
        name="kv_project",
        cost_estimate=pl.CostEstimate(
            flops=2 * tok_count * width * 2 * LANES, bytes_accessed=4 * tok_count * width, transcendentals=0
        ),
    )(owner_t, part_t, tokens, key_weight, value_weight, coarse, fine)
    kv_rows, sent = kv_out[0], list(kv_out[1:])

    mine_owner = lax.dynamic_slice_in_dim(owner_t, me * qblocks, qblocks, 1)
    if direct:
        gathered = []
        for at, (_, shift, _) in enumerate(plan):
            if shift:
                pairs = [(i, i + shift) for i in range(devices - shift)]
                gathered.append(lax.ppermute(sent[at], "kv", pairs))
            else:
                gathered.append(sent[at])
        by_group = [gathered[g::groups] for g in range(groups)]
        wanted = me - jnp.arange(devices, dtype=jnp.int32)
        valid = jnp.any(mine_owner[:, :, None] == jnp.where(wanted < 0, -2, wanted), axis=0)
        valid = valid.astype(jnp.int32)
    else:
        got = lax.all_to_all(
            sent[0].reshape(devices, qblocks, KEY_BLOCK, 2 * LANES),
            "kv",
            split_axis=0,
            concat_axis=0,
            tiled=True,
        )
        rows = jnp.arange(qblocks, dtype=jnp.int32)
        picks = [got[jnp.maximum(mine_owner[slot], 0), rows] for slot in range(chosen)]
        by_group = [
            [p[g * per_group : (g + 1) * per_group] for p in picks] for g in range(groups)
        ]
        valid = (mine_owner.T >= 0).astype(jnp.int32)
    sources = valid.shape[1]

    q_rows = 256
    queries = pl.pallas_call(
        q_kernel,
        grid=(tok_count // q_rows,),
        out_shape=jax.ShapeDtypeStruct((tok_count, heads * LANES), BF16),
        in_specs=[
            pl.BlockSpec((1, q_rows, width), lambda i: (0, i, 0)),
            pl.BlockSpec((width, heads * HEAD_DIM), lambda i: (0, 0)),
            vm,
            vm,
        ],
        out_specs=pl.BlockSpec((q_rows, heads * LANES), lambda i: (i, 0)),
        name="q_project",
        cost_estimate=pl.CostEstimate(
            flops=2 * tok_count * width * heads * HEAD_DIM,
            bytes_accessed=4 * tok_count * width,
            transcendentals=0,
        ),
    )(tokens, query_weight, coarse, fine)
    other_weight = lax.ppermute(out_weight, "tp", swap)

    results = []
    gain = norm_gain.reshape(1, -1)
    cols = norm_gain.shape[0]
    depth = heads * HEAD_DIM
    for g in range(groups):
        at0 = g * per_group
        mixed = pl.pallas_call(
            functools.partial(attention_kernel, sources),
            grid=(per_group,),
            out_shape=jax.ShapeDtypeStruct((per_group * QUERY_BLOCK, depth), BF16),
            in_specs=[
                sm,
                pl.BlockSpec((QUERY_BLOCK, heads * LANES), lambda i, at0=at0: (at0 + i, 0)),
                pl.BlockSpec(
                    (QUERY_BLOCK // KEY_BLOCK, KEY_BLOCK, 2 * LANES), lambda i, at0=at0: (at0 + i, 0, 0)
                ),
            ]
            + [pl.BlockSpec((1, KEY_BLOCK, 2 * LANES), lambda i: (i, 0, 0))] * sources,
            out_specs=pl.BlockSpec((QUERY_BLOCK, depth), lambda i: (i, 0)),
            name=f"attend_{g}",
            cost_estimate=pl.CostEstimate(
                flops=4 * per_group * QUERY_BLOCK * heads * LANES * (sources * KEY_BLOCK + QUERY_BLOCK),
                bytes_accessed=per_group * QUERY_BLOCK * depth * 6,
                transcendentals=0,
            ),
        )(valid[at0 : at0 + per_group], queries, kv_rows, *by_group[g])
        other_mixed = lax.ppermute(mixed, "tp", swap)
        o_rows = 128
        results.append(
            pl.pallas_call(
                out_kernel,
                grid=(per_group * QUERY_BLOCK // o_rows,),
                out_shape=jax.ShapeDtypeStruct((per_group * QUERY_BLOCK, cols), BF16),
                in_specs=[
                    pl.BlockSpec((o_rows, depth), lambda i: (i, 0)),
                    pl.BlockSpec((o_rows, depth), lambda i: (i, 0)),
                    hb,
                    hb,
                    pl.BlockSpec((1, cols), lambda i: (0, 0)),
                ],
                out_specs=pl.BlockSpec((o_rows, cols), lambda i: (i, 0)),
                scratch_shapes=[
                    pltpu.VMEM((2, depth, 2 * cols), BF16),
                    pltpu.SemaphoreType.DMA((2, heads)),
                ],
                name=f"project_{g}",
                cost_estimate=pl.CostEstimate(
                    flops=8 * per_group * QUERY_BLOCK * depth * cols,
                    bytes_accessed=8 * depth * cols,
                    transcendentals=0,
                ),
            )(mixed, other_mixed, out_weight, other_weight, gain)
        )
    result = results[0] if groups == 1 else jnp.concatenate(results, axis=0)
    return result[None]


def solution(mesh):
    placed = (
        P("dp", "kv", None),
        P(None, "tp"),
        P(None, "tp"),
        P(None, "tp"),
        P("tp", None),
        P("tp"),
        P("dp", None, None),
        P("dp", None, None),
    )
    return jax.shard_map(
        body, mesh=mesh, in_specs=placed, out_specs=P("dp", "kv", "tp"), check_vma=False
    )
```

```python
import functools

import jax
import jax.numpy as jnp
import numpy as np
from jax import lax
from jax.experimental import pallas as pl
from jax.experimental.pallas import tpu as pltpu
from jax.sharding import PartitionSpec as P


HEAD_DIM = 64
QUERY_BLOCK = 128
KEY_BLOCK = 64
LANES = 128
ROPE_BASE = 10000.0
NORM_EPS = 1e-06
LOG2E = 1.4426950408889634
GROUPS = (3, 3)
PER_DOT = 2
OUT_SPLIT = 2


BF16 = jnp.bfloat16
F32 = jnp.float32
HBM = pltpu.MemorySpace.HBM
VMEM = pltpu.MemorySpace.VMEM


def angle_tables(length):
    half = HEAD_DIM // 2
    frequency = ROPE_BASE ** (-np.arange(half, dtype=np.float64) / half)
    lane_frequency = np.tile(frequency, LANES // half)
    sign = np.tile(np.repeat([-1.0, 1.0], half), LANES // HEAD_DIM)
    coarse = (np.arange(length // KEY_BLOCK) * KEY_BLOCK)[:, None] * lane_frequency
    fine = np.arange(KEY_BLOCK)[:, None] * lane_frequency
    make = lambda a: np.stack([np.cos(a), np.sin(a) * sign], 1).astype(np.float32)
    return make(coarse), np.swapaxes(make(fine), 0, 1).copy()


def rotate_tile(tile, cosine, sine):
    lane = lax.broadcasted_iota(jnp.int32, tile.shape, 1)
    half = HEAD_DIM // 2
    first = (lane % HEAD_DIM) < half
    swapped = jnp.where(
        first, pltpu.roll(tile, LANES - half, 1), pltpu.roll(tile, half, 1)
    )
    return tile * cosine + swapped * sine


def block_angles(coarse_ref, fine_ref, block):
    coarse = coarse_ref[block]
    c_a, s_a = coarse[0:1], coarse[1:2]
    c_b, s_b = fine_ref[0], fine_ref[1]
    return c_a * c_b - s_a * s_b, s_a * c_b + c_a * s_b


def wanted_block(owner_ref, part_ref, row, me):
    total = jnp.int32(0)
    for slot in range(owner_ref.shape[0]):
        total = total + jnp.where(owner_ref[slot, row] == me, part_ref[slot, row], 0)
    return total


def kv_kernel(plan, chunk, *refs):
    owner_hbm, part_hbm, tokens_ref, wk_ref, wv_ref, coarse_hbm, fine_hbm = refs[:7]
    kv_ref, bias_ref, tok = refs[7:10]
    send_refs = refs[10 : 10 + len(plan)]
    weight, coarse_ref, fine_ref, owner_ref, part_ref, tok_sem, sem = refs[10 + len(plan) :]
    rows = tok.shape[0]
    me = lax.axis_index("kv")
    per_chunk = chunk // KEY_BLOCK
    blocks = rows // KEY_BLOCK
    qblocks = rows // QUERY_BLOCK
    small = [
        (wk_ref, weight.at[:, pl.ds(0, LANES)]),
        (wv_ref, weight.at[:, pl.ds(LANES, LANES)]),
        (coarse_hbm.at[pl.ds(me * blocks, blocks)], coarse_ref),
        (fine_hbm, fine_ref),
        (owner_hbm, owner_ref),
        (part_hbm, part_ref),
    ]
    small = [pltpu.make_async_copy(src, dst, sem.at[at]) for at, (src, dst) in enumerate(small)]
    t_copies = [
        pltpu.make_async_copy(
            tokens_ref.at[0, pl.ds(at * chunk, chunk)], tok.at[pl.ds(at * chunk, chunk)], tok_sem.at[at]
        )
        for at in range(rows // chunk)
    ]
    for copy in small[:2] + t_copies[:1] + small[2:] + t_copies[1:]:
        copy.start()
    for copy in small:
        copy.wait()
    for at in range(rows // chunk):
        t_copies[at].wait()
        product = jnp.dot(
            tok[pl.ds(at * chunk, chunk)], weight[...], preferred_element_type=F32
        )
        for sub in range(per_chunk):
            block = at * per_chunk + sub
            cosine, sine = block_angles(coarse_ref, fine_ref, block)
            piece = product[sub * KEY_BLOCK : (sub + 1) * KEY_BLOCK]
            kv_ref[block, :, 0:LANES] = rotate_tile(piece[:, :LANES], cosine, sine).astype(BF16)
            kv_ref[block, :, LANES : 2 * LANES] = piece[:, LANES:].astype(BF16)
    for (kind, arg, first), out in zip(plan, send_refs):
        if kind == "pair":
            target = me ^ arg
            for row in range(out.shape[0]):
                out[row] = kv_ref[wanted_block(owner_ref, part_ref, target * qblocks + first + row, me)]
        else:
            def fill(index, carry, out=out):
                out[index] = kv_ref[wanted_block(owner_ref, part_ref, index, me)]
                return carry
            lax.fori_loop(0, out.shape[0], fill, 0)
    far = bias_ref.shape[2]
    source_id = lax.broadcasted_iota(jnp.int32, (1, far), 1) // KEY_BLOCK
    for row in range(qblocks):
        owners = [owner_ref[slot, me * qblocks + row] for slot in range(owner_ref.shape[0])]
        if plan[0][0] == "pair":
            wanted = me ^ source_id
            named = functools.reduce(
                jnp.logical_or, [wanted == owner for owner in owners]
            )
        else:
            named = functools.reduce(
                jnp.logical_or,
                [jnp.logical_and(source_id == at, owner >= 0) for at, owner in enumerate(owners)],
            )
        bias_ref[row] = jnp.where(named, jnp.float32(0), jnp.float32(-jnp.inf))


def q_kernel(chunk, tok_ref, weight_ref, coarse_ref, fine_ref, out_ref):
    rows, tiles = tok_ref.shape[0], weight_ref.shape[1] // LANES
    blocks = rows // KEY_BLOCK
    me = lax.axis_index("kv")
    low = lax.broadcasted_iota(jnp.int32, (KEY_BLOCK, LANES), 1) < HEAD_DIM
    per_chunk = chunk // KEY_BLOCK
    for at in range(rows // chunk):
        product = jnp.dot(
            tok_ref[at * chunk : (at + 1) * chunk], weight_ref[...], preferred_element_type=F32
        ) * (HEAD_DIM ** -0.5)
        for sub in range(per_chunk):
            block = at * per_chunk + sub
            cosine, sine = block_angles(coarse_ref, fine_ref, me * blocks + block)
            span = slice(block * KEY_BLOCK, (block + 1) * KEY_BLOCK)
            for tile in range(tiles):
                piece = rotate_tile(
                    product[sub * KEY_BLOCK : (sub + 1) * KEY_BLOCK, tile * LANES : (tile + 1) * LANES],
                    cosine,
                    sine,
                )
                other = pltpu.roll(piece, HEAD_DIM, 1)
                if tile < tiles // 2:
                    even, odd = jnp.where(low, piece, 0.0), jnp.where(low, other, 0.0)
                else:
                    even, odd = jnp.where(low, 0.0, other), jnp.where(low, 0.0, piece)
                out_ref[2 * tile, span] = even.astype(BF16)
                out_ref[2 * tile + 1, span] = odd.astype(BF16)


def attention_kernel(first, sources, per_dot, q_ref, own_ref, bias_ref, *refs):
    source_refs, out_ref = refs[:sources], refs[-1]
    heads = q_ref.shape[0]
    pairs = heads // 2
    far = sources * KEY_BLOCK
    row_id = lax.broadcasted_iota(jnp.int32, (QUERY_BLOCK, QUERY_BLOCK), 0)
    col_id = lax.broadcasted_iota(jnp.int32, (QUERY_BLOCK, QUERY_BLOCK), 1)
    lower = row_id >= col_id
    low = lax.broadcasted_iota(jnp.int32, (QUERY_BLOCK, LANES), 1) < HEAD_DIM
    per_query = QUERY_BLOCK // KEY_BLOCK
    for row in range(out_ref.shape[0] // QUERY_BLOCK):
        block = first + row
        picks = [ref[row] for ref in source_refs]
        picks += [own_ref[block * per_query + at] for at in range(per_query)]
        keys = jnp.concatenate([p[:, :LANES] for p in picks], axis=0)
        values = jnp.concatenate([p[:, LANES:] for p in picks], axis=0)
        values = jnp.concatenate([values, jnp.ones_like(values)], axis=1)
        bias = bias_ref[block]
        span = pl.ds(block * QUERY_BLOCK, QUERY_BLOCK)
        for start in range(0, pairs, per_dot):
            order = [h for p in range(start, start + per_dot) for h in (p, p + pairs)]
            query = jnp.concatenate([q_ref[h, span] for h in order], axis=0)
            scores = lax.dot_general(
                query, keys, (((1,), (1,)), ((), ())), preferred_element_type=F32
            )
            parts = []
            for at in range(len(order)):
                piece = scores[at * QUERY_BLOCK : (at + 1) * QUERY_BLOCK]
                piece = jnp.concatenate(
                    [piece[:, :far] + bias, jnp.where(lower, piece[:, far:], -jnp.inf)], axis=1
                )
                row_max = jnp.max(piece, axis=1, keepdims=True)
                parts.append(jnp.exp2((piece - row_max) * LOG2E).astype(BF16))
            mixed = jnp.dot(jnp.concatenate(parts, axis=0), values, preferred_element_type=F32)
            for at in range(per_dot):
                one = mixed[2 * at * QUERY_BLOCK : (2 * at + 1) * QUERY_BLOCK]
                two = mixed[(2 * at + 1) * QUERY_BLOCK : (2 * at + 2) * QUERY_BLOCK]
                top = jnp.where(low, one[:, :LANES], two[:, :LANES])
                bottom = jnp.where(low, one[:, LANES:], two[:, LANES:])
                out_ref[
                    row * QUERY_BLOCK : (row + 1) * QUERY_BLOCK, (start + at) * LANES : (start + at + 1) * LANES
                ] = (top / bottom).astype(BF16)


def out_kernel(first, split, mine_ref, other_ref, w_mine_ref, w_other_ref, gain_ref, *refs):
    out_hbm, kept, staged, sem = refs[-4:]
    rows, cols = staged.shape
    depth = w_mine_ref.shape[0]
    heads = depth // HEAD_DIM
    me = lax.axis_index("tp")
    width = 256
    order = [h for p in range(heads // 2) for h in (p, p + heads // 2)]
    tile = rows // split
    copies = []
    for part in range(split):
        span = slice(part * tile, (part + 1) * tile)
        mine, other = mine_ref[span], other_ref[span]
        total = None
        for half in range(2):
            for at in range(cols // width):
                start = pl.multiple_of((me if half == 0 else 1 - me) * cols + at * width, width)
                load = lambda ref: jnp.concatenate(
                    [ref[h * HEAD_DIM : (h + 1) * HEAD_DIM, pl.ds(start, width)] for h in order], axis=0
                )
                a = jnp.dot(mine, load(w_mine_ref), preferred_element_type=F32)
                b = jnp.dot(other, load(w_other_ref), preferred_element_type=F32)
                projected = a.astype(BF16).astype(F32) + b.astype(BF16).astype(F32)
                if half == 0:
                    kept[span, at * width : (at + 1) * width] = projected
                squares = projected * projected
                squares = squares[:, :LANES] + squares[:, LANES:]
                total = squares if total is None else total + squares
        total = jnp.sum(total, axis=1, keepdims=True)
        scale = lax.rsqrt(total / (2 * cols) + NORM_EPS)
        for at in range(cols // width):
            put = slice(at * width, (at + 1) * width)
            staged[span, put] = (kept[span, put] * scale * gain_ref[:, put]).astype(BF16)
        copies.append(
            pltpu.make_async_copy(
                staged.at[pl.ds(part * tile, tile)],
                out_hbm.at[0, pl.ds(first * QUERY_BLOCK + part * tile, tile)],
                sem.at[part],
            )
        )
        copies[-1].start()
    for copy in copies:
        copy.wait()


def body(
    tokens, query_weight, key_weight, value_weight, out_weight, norm_gain, chosen_owner, chosen_part
):
    tok_count, width = tokens.shape[1], tokens.shape[2]
    devices = lax.axis_size("kv")
    me = lax.axis_index("kv")
    heads = query_weight.shape[1] // HEAD_DIM
    assert key_weight.shape[1] == LANES and value_weight.shape[1] == LANES
    per_device = tok_count // KEY_BLOCK
    qblocks = tok_count // QUERY_BLOCK
    owner_t, part_t = chosen_owner[0].T, chosen_part[0].T
    chosen = owner_t.shape[0]
    coarse, fine = (jnp.asarray(t) for t in angle_tables(devices * tok_count))
    swap = [(0, 1), (1, 0)]
    vm = pl.BlockSpec(memory_space=VMEM)
    hb = pl.BlockSpec(memory_space=HBM)
    direct = devices <= chosen and devices & (devices - 1) == 0
    resident = functools.partial(pltpu.with_memory_space_constraint, memory_space=VMEM)
    distant = functools.partial(pltpu.with_memory_space_constraint, memory_space=HBM)

    sizes = GROUPS if direct and sum(GROUPS) == qblocks else (qblocks,)
    firsts = [sum(sizes[:g]) for g in range(len(sizes))]
    sources = devices if direct else chosen
    plan = (
        [("pair", pair, firsts[g]) for g in range(len(sizes)) for pair in range(devices)]
        if direct
        else [("all", 0, 0)]
    )
    block_shape = (KEY_BLOCK, 2 * LANES)
    sends = (
        [pltpu.VMEM((sizes[g],) + block_shape, BF16) for g in range(len(sizes)) for _ in range(devices)]
        if direct
        else [jax.ShapeDtypeStruct((devices * qblocks,) + block_shape, BF16)]
    )
    chunk = 256
    table_scratch = [pltpu.VMEM((per_device, 2, LANES), F32), pltpu.VMEM((2, KEY_BLOCK, LANES), F32)]
    kv_out = pl.pallas_call(
        functools.partial(kv_kernel, plan, chunk),
        out_shape=[
            pltpu.VMEM((per_device,) + block_shape, BF16),
            pltpu.VMEM((qblocks, 1, sources * KEY_BLOCK), F32),
            pltpu.VMEM((tok_count, width), BF16),
        ]
        + sends,
        in_specs=[hb] * 7,
        out_specs=[vm] * (3 + len(sends)),
        scratch_shapes=[
            pltpu.VMEM((width, 2 * LANES), BF16),
            *table_scratch,
            pltpu.SMEM(owner_t.shape, jnp.int32),
            pltpu.SMEM(part_t.shape, jnp.int32),
            pltpu.SemaphoreType.DMA((tok_count // chunk,)),
            pltpu.SemaphoreType.DMA((6,)),
        ],
        compiler_params=pltpu.CompilerParams(vmem_limit_bytes=24 << 20),
        name="kv_project",
        cost_estimate=pl.CostEstimate(
            flops=2 * tok_count * width * 2 * LANES, bytes_accessed=4 * tok_count * width, transcendentals=0
        ),
    )(*map(distant, (owner_t, part_t, tokens, key_weight, value_weight, coarse, fine)))
    kv_rows, bias, loaded, sent = kv_out[0], kv_out[1], kv_out[2], list(kv_out[3:])

    if direct:
        by_group = []
        for g in range(len(sizes)):
            arrived = []
            for pair in range(devices):
                block = sent[g * devices + pair]
                if pair:
                    block = lax.ppermute(block, "kv", [(i, i ^ pair) for i in range(devices)])
                arrived.append(resident(block))
            by_group.append(arrived)
    else:
        got = lax.all_to_all(
            sent[0].reshape((devices, qblocks) + block_shape), "kv", split_axis=0, concat_axis=0, tiled=True
        )
        mine_owner = lax.dynamic_slice_in_dim(owner_t, me * qblocks, qblocks, 1)
        rows = jnp.arange(qblocks, dtype=jnp.int32)
        by_group = [[got[jnp.maximum(mine_owner[slot], 0), rows] for slot in range(chosen)]]

    queries = pl.pallas_call(
        functools.partial(q_kernel, chunk),
        out_shape=pltpu.VMEM((heads, tok_count, LANES), BF16),
        in_specs=[vm] * 4,
        out_specs=vm,
        compiler_params=pltpu.CompilerParams(vmem_limit_bytes=24 << 20),
        name="q_project",
        cost_estimate=pl.CostEstimate(
            flops=2 * tok_count * width * heads * HEAD_DIM,
            bytes_accessed=4 * tok_count * width,
            transcendentals=0,
        ),
    )(*map(resident, (loaded, query_weight, coarse, fine)))
    other_weight = resident(lax.ppermute(out_weight, "tp", swap))
    my_weight = resident(out_weight)

    gain = norm_gain.reshape(1, -1)
    cols = norm_gain.shape[0]
    depth = heads * HEAD_DIM
    result = None
    for g, (first, size) in enumerate(zip(firsts, sizes)):
        tokens_here = size * QUERY_BLOCK
        extra = [] if result is None else [result]
        mixed = pl.pallas_call(
            functools.partial(attention_kernel, first, sources, PER_DOT),
            out_shape=pltpu.VMEM((tokens_here, depth), BF16),
            in_specs=[vm] * (3 + sources) + [hb] * len(extra),
            out_specs=vm,
            compiler_params=pltpu.CompilerParams(vmem_limit_bytes=24 << 20),
            cost_estimate=pl.CostEstimate(
                flops=4 * tokens_here * heads * LANES * (sources * KEY_BLOCK + QUERY_BLOCK),
                bytes_accessed=tokens_here * depth * 6,
                transcendentals=0,
            ),
        )(resident(queries), resident(kv_rows), resident(bias), *by_group[g], *map(distant, extra))
        other_mixed = resident(lax.ppermute(mixed, "tp", swap))
        split = OUT_SPLIT
        result = pl.pallas_call(
            functools.partial(out_kernel, first, split),
            out_shape=jax.ShapeDtypeStruct((1, tok_count, cols), BF16),
            in_specs=[vm, vm, vm, vm, vm] + [hb] * len(extra),
            out_specs=hb,
            input_output_aliases={5: 0} if extra else {},
            scratch_shapes=[
                pltpu.VMEM((tokens_here, cols), F32),
                pltpu.VMEM((tokens_here, cols), BF16),
                pltpu.SemaphoreType.DMA((split,)),
            ],
            compiler_params=pltpu.CompilerParams(vmem_limit_bytes=24 << 20),
            cost_estimate=pl.CostEstimate(
                flops=8 * tokens_here * depth * cols,
                bytes_accessed=8 * depth * cols,
                transcendentals=0,
            ),
        )(resident(mixed), other_mixed, my_weight, other_weight, gain, *map(distant, extra))
    return result


def solution(mesh):
    placed = (
        P("dp", "kv", None),
        P(None, "tp"),
        P(None, "tp"),
        P(None, "tp"),
        P("tp", None),
        P("tp"),
        P("dp", None, None),
        P("dp", None, None),
    )
    return jax.shard_map(body, mesh=mesh, in_specs=placed, out_specs=P("dp", "kv", "tp"), check_vma=False)
```

```python
import functools

import jax
import jax.numpy as jnp
import numpy as np
from jax import lax
from jax.experimental import pallas as pl
from jax.experimental.pallas import tpu as pltpu
from jax.sharding import PartitionSpec as P


HEAD_DIM = 64
QUERY_BLOCK = 128
KEY_BLOCK = 64
LANES = 128
ROPE_BASE = 10000.0
NORM_EPS = 1e-06
LOG2E = 1.4426950408889634
GROUPS = (3, 3)
PER_DOT = 4
OUT_SPLIT = 2


BF16 = jnp.bfloat16
F32 = jnp.float32
HBM = pltpu.MemorySpace.HBM
VMEM = pltpu.MemorySpace.VMEM


def angle_tables(length):
    half = HEAD_DIM // 2
    frequency = ROPE_BASE ** (-np.arange(half, dtype=np.float64) / half)
    lane_frequency = np.tile(frequency, LANES // half)
    sign = np.tile(np.repeat([-1.0, 1.0], half), LANES // HEAD_DIM)
    coarse = (np.arange(length // KEY_BLOCK) * KEY_BLOCK)[:, None] * lane_frequency
    fine = np.arange(KEY_BLOCK)[:, None] * lane_frequency
    make = lambda a: np.stack([np.cos(a), np.sin(a) * sign], 1).astype(np.float32)
    return make(coarse), np.swapaxes(make(fine), 0, 1).copy()


def rotate_tile(tile, cosine, sine):
    lane = lax.broadcasted_iota(jnp.int32, tile.shape, 1)
    half = HEAD_DIM // 2
    first = (lane % HEAD_DIM) < half
    swapped = jnp.where(
        first, pltpu.roll(tile, LANES - half, 1), pltpu.roll(tile, half, 1)
    )
    return tile * cosine + swapped * sine


def block_angles(coarse_ref, fine_ref, block):
    coarse = coarse_ref[block]
    c_a, s_a = coarse[0:1], coarse[1:2]
    c_b, s_b = fine_ref[0], fine_ref[1]
    return c_a * c_b - s_a * s_b, s_a * c_b + c_a * s_b


def wanted_block(owner_ref, part_ref, row, me):
    total = jnp.int32(0)
    for slot in range(owner_ref.shape[0]):
        total = total + jnp.where(owner_ref[slot, row] == me, part_ref[slot, row], 0)
    return total


def kv_kernel(plan, chunk, *refs):
    owner_hbm, part_hbm, tokens_ref, wk_ref, wv_ref, coarse_hbm, fine_hbm, wq_hbm, wo_hbm = refs[:9]
    kv_ref, bias_ref, tok, coarse_ref, fine_ref, wq_ref, wo_ref = refs[9:16]
    send_refs = refs[16 : 16 + len(plan)]
    weight, owner_ref, part_ref, tok_sem, sem = refs[16 + len(plan) :]
    rows = tok.shape[0]
    me = lax.axis_index("kv")
    per_chunk = chunk // KEY_BLOCK
    blocks = rows // KEY_BLOCK
    qblocks = rows // QUERY_BLOCK
    small = [
        (wk_ref, weight.at[:, pl.ds(0, LANES)]),
        (wv_ref, weight.at[:, pl.ds(LANES, LANES)]),
        (coarse_hbm.at[pl.ds(me * blocks, blocks)], coarse_ref),
        (fine_hbm, fine_ref),
        (owner_hbm, owner_ref),
        (part_hbm, part_ref),
        (wq_hbm, wq_ref),
        (wo_hbm, wo_ref),
    ]
    small = [pltpu.make_async_copy(src, dst, sem.at[at]) for at, (src, dst) in enumerate(small)]
    t_copies = [
        pltpu.make_async_copy(
            tokens_ref.at[0, pl.ds(at * chunk, chunk)], tok.at[pl.ds(at * chunk, chunk)], tok_sem.at[at]
        )
        for at in range(rows // chunk)
    ]
    small, later = small[:-2], small[-2:]
    for copy in small[:2] + t_copies[:1] + small[2:] + t_copies[1:] + later:
        copy.start()
    for copy in small:
        copy.wait()
    for at in range(rows // chunk):
        t_copies[at].wait()
        product = jnp.dot(
            tok[pl.ds(at * chunk, chunk)], weight[...], preferred_element_type=F32
        )
        for sub in range(per_chunk):
            block = at * per_chunk + sub
            cosine, sine = block_angles(coarse_ref, fine_ref, block)
            piece = product[sub * KEY_BLOCK : (sub + 1) * KEY_BLOCK]
            kv_ref[block, :, 0:LANES] = rotate_tile(piece[:, :LANES], cosine, sine).astype(BF16)
            kv_ref[block, :, LANES : 2 * LANES] = piece[:, LANES:].astype(BF16)
    for (kind, arg, first), out in zip(plan, send_refs):
        if kind == "pair":
            target = me ^ arg
            for row in range(out.shape[0]):
                out[row] = kv_ref[wanted_block(owner_ref, part_ref, target * qblocks + first + row, me)]
        else:
            def fill(index, carry, out=out):
                out[index] = kv_ref[wanted_block(owner_ref, part_ref, index, me)]
                return carry
            lax.fori_loop(0, out.shape[0], fill, 0)
    far = bias_ref.shape[2]
    source_id = lax.broadcasted_iota(jnp.int32, (1, far), 1) // KEY_BLOCK
    for row in range(qblocks):
        owners = [owner_ref[slot, me * qblocks + row] for slot in range(owner_ref.shape[0])]
        if plan[0][0] == "pair":
            wanted = me ^ source_id
            named = functools.reduce(
                jnp.logical_or, [wanted == owner for owner in owners]
            )
        else:
            named = functools.reduce(
                jnp.logical_or,
                [jnp.logical_and(source_id == at, owner >= 0) for at, owner in enumerate(owners)],
            )
        bias_ref[row] = jnp.where(named, jnp.float32(0), jnp.float32(-jnp.inf))
    for copy in later:
        copy.wait()


def q_kernel(chunk, tok_ref, weight_ref, coarse_ref, fine_ref, out_ref):
    rows, tiles = tok_ref.shape[0], weight_ref.shape[1] // LANES
    low = lax.broadcasted_iota(jnp.int32, (KEY_BLOCK, LANES), 1) < HEAD_DIM
    per_chunk = chunk // KEY_BLOCK
    for at in range(rows // chunk):
        product = jnp.dot(
            tok_ref[at * chunk : (at + 1) * chunk], weight_ref[...], preferred_element_type=F32
        ) * (HEAD_DIM ** -0.5)
        for sub in range(per_chunk):
            block = at * per_chunk + sub
            cosine, sine = block_angles(coarse_ref, fine_ref, block)
            span = slice(block * KEY_BLOCK, (block + 1) * KEY_BLOCK)
            for tile in range(tiles):
                piece = rotate_tile(
                    product[sub * KEY_BLOCK : (sub + 1) * KEY_BLOCK, tile * LANES : (tile + 1) * LANES],
                    cosine,
                    sine,
                )
                other = pltpu.roll(piece, HEAD_DIM, 1)
                if tile < tiles // 2:
                    even, odd = jnp.where(low, piece, 0.0), jnp.where(low, other, 0.0)
                else:
                    even, odd = jnp.where(low, 0.0, other), jnp.where(low, 0.0, piece)
                out_ref[2 * tile, span] = even.astype(BF16)
                out_ref[2 * tile + 1, span] = odd.astype(BF16)


def attention_kernel(first, offsets, per_dot, q_ref, own_ref, bias_ref, *refs):
    sources = len(offsets)
    source_refs, out_ref = refs[:sources], refs[-1]
    heads = q_ref.shape[0]
    pairs = heads // 2
    far = sources * KEY_BLOCK
    row_id = lax.broadcasted_iota(jnp.int32, (QUERY_BLOCK, QUERY_BLOCK), 0)
    col_id = lax.broadcasted_iota(jnp.int32, (QUERY_BLOCK, QUERY_BLOCK), 1)
    lower = row_id >= col_id
    low = lax.broadcasted_iota(jnp.int32, (QUERY_BLOCK, LANES), 1) < HEAD_DIM
    per_query = QUERY_BLOCK // KEY_BLOCK
    for row in range(out_ref.shape[0] // QUERY_BLOCK):
        block = first + row
        picks = [ref[offset + row] for ref, offset in zip(source_refs, offsets)]
        picks += [own_ref[block * per_query + at] for at in range(per_query)]
        keys = jnp.concatenate([p[:, :LANES] for p in picks], axis=0)
        values = jnp.concatenate([p[:, LANES:] for p in picks], axis=0)
        values = jnp.concatenate([values, jnp.ones_like(values)], axis=1)
        bias = bias_ref[block]
        span = pl.ds(block * QUERY_BLOCK, QUERY_BLOCK)
        for start in range(0, pairs, per_dot):
            order = [h for p in range(start, start + per_dot) for h in (p, p + pairs)]
            query = jnp.concatenate([q_ref[h, span] for h in order], axis=0)
            scores = lax.dot_general(
                query, keys, (((1,), (1,)), ((), ())), preferred_element_type=F32
            )
            parts = []
            for at in range(len(order)):
                piece = scores[at * QUERY_BLOCK : (at + 1) * QUERY_BLOCK]
                piece = jnp.concatenate(
                    [piece[:, :far] + bias, jnp.where(lower, piece[:, far:], -jnp.inf)], axis=1
                )
                row_max = jnp.max(piece, axis=1, keepdims=True)
                parts.append(jnp.exp2((piece - row_max) * LOG2E).astype(BF16))
            mixed = jnp.dot(jnp.concatenate(parts, axis=0), values, preferred_element_type=F32)
            for at in range(per_dot):
                one = mixed[2 * at * QUERY_BLOCK : (2 * at + 1) * QUERY_BLOCK]
                two = mixed[(2 * at + 1) * QUERY_BLOCK : (2 * at + 2) * QUERY_BLOCK]
                top = jnp.where(low, one[:, :LANES], two[:, :LANES])
                bottom = jnp.where(low, one[:, LANES:], two[:, LANES:])
                out_ref[
                    row * QUERY_BLOCK : (row + 1) * QUERY_BLOCK, (start + at) * LANES : (start + at + 1) * LANES
                ] = (top / bottom).astype(BF16)


def column_start(half, me, cols, at, width):
    return pl.multiple_of((me if half == 0 else 1 - me) * cols + at * width, width)


def weight_columns(ref, start, width):
    heads = ref.shape[0] // HEAD_DIM
    order = [h for p in range(heads // 2) for h in (p, p + heads // 2)]
    return jnp.concatenate(
        [ref[h * HEAD_DIM : (h + 1) * HEAD_DIM, pl.ds(start, width)] for h in order], axis=0
    )


def partial_kernel(mine_ref, weight_ref, out_ref):
    width = 256
    mine = mine_ref[...]
    for at in range(out_ref.shape[1] // width):
        span = slice(at * width, (at + 1) * width)
        out_ref[:, span] = jnp.dot(
            mine, weight_columns(weight_ref, at * width, width), preferred_element_type=F32
        ).astype(BF16)


def out_kernel(first, split, partial_ref, other_ref, weight_ref, gain_ref, *refs):
    out_hbm, kept, staged, sem = refs[-4:]
    rows, cols = staged.shape
    me = lax.axis_index("tp")
    width = 256
    tile = rows // split
    copies = []
    for part in range(split):
        span = slice(part * tile, (part + 1) * tile)
        other = other_ref[span]
        total = None
        for half in range(2):
            for at in range(cols // width):
                start = column_start(half, me, cols, at, width)
                theirs = jnp.dot(
                    other, weight_columns(weight_ref, start, width), preferred_element_type=F32
                )
                mine = partial_ref[span, pl.ds(start, width)].astype(F32)
                projected = mine + theirs.astype(BF16).astype(F32)
                if half == 0:
                    kept[span, at * width : (at + 1) * width] = projected
                squares = projected * projected
                squares = squares[:, :LANES] + squares[:, LANES:]
                total = squares if total is None else total + squares
        total = jnp.sum(total, axis=1, keepdims=True)
        scale = lax.rsqrt(total / (2 * cols) + NORM_EPS)
        for at in range(cols // width):
            put = slice(at * width, (at + 1) * width)
            staged[span, put] = (kept[span, put] * scale * gain_ref[:, put]).astype(BF16)
        copies.append(
            pltpu.make_async_copy(
                staged.at[pl.ds(part * tile, tile)],
                out_hbm.at[0, pl.ds(first * QUERY_BLOCK + part * tile, tile)],
                sem.at[part],
            )
        )
        copies[-1].start()
    for copy in copies:
        copy.wait()


def body(
    tokens, query_weight, key_weight, value_weight, out_weight, norm_gain, chosen_owner, chosen_part
):
    tok_count, width = tokens.shape[1], tokens.shape[2]
    devices = lax.axis_size("kv")
    me = lax.axis_index("kv")
    heads = query_weight.shape[1] // HEAD_DIM
    assert key_weight.shape[1] == LANES and value_weight.shape[1] == LANES
    per_device = tok_count // KEY_BLOCK
    qblocks = tok_count // QUERY_BLOCK
    owner_t, part_t = chosen_owner[0].T, chosen_part[0].T
    chosen = owner_t.shape[0]
    coarse, fine = (jnp.asarray(t) for t in angle_tables(devices * tok_count))
    swap = [(0, 1), (1, 0)]
    vm = pl.BlockSpec(memory_space=VMEM)
    hb = pl.BlockSpec(memory_space=HBM)
    direct = devices <= chosen and devices & (devices - 1) == 0
    resident = functools.partial(pltpu.with_memory_space_constraint, memory_space=VMEM)
    distant = functools.partial(pltpu.with_memory_space_constraint, memory_space=HBM)

    sizes = GROUPS if direct and sum(GROUPS) == qblocks else (qblocks,)
    firsts = [sum(sizes[:g]) for g in range(len(sizes))]
    sources = devices if direct else chosen
    whole = (0, 1) if len(sizes) > 1 else ()
    pieces = [(pair, None) for pair in whole]
    pieces += [(pair, g) for g in range(len(sizes)) for pair in range(devices) if pair not in whole]
    extent = lambda g: (0, qblocks) if g is None else (firsts[g], sizes[g])
    plan = [("pair", pair, extent(g)[0]) for pair, g in pieces] if direct else [("all", 0, 0)]
    block_shape = (KEY_BLOCK, 2 * LANES)
    sends = (
        [pltpu.VMEM((extent(g)[1],) + block_shape, BF16) for _, g in pieces]
        if direct
        else [jax.ShapeDtypeStruct((devices * qblocks,) + block_shape, BF16)]
    )
    chunk = 256
    kv_out = pl.pallas_call(
        functools.partial(kv_kernel, plan, chunk),
        out_shape=[
            pltpu.VMEM((per_device,) + block_shape, BF16),
            pltpu.VMEM((qblocks, 1, sources * KEY_BLOCK), F32),
            pltpu.VMEM((tok_count, width), BF16),
            pltpu.VMEM((per_device, 2, LANES), F32),
            pltpu.VMEM((2, KEY_BLOCK, LANES), F32),
            pltpu.VMEM(query_weight.shape, BF16),
            pltpu.VMEM(out_weight.shape, BF16),
        ]
        + sends,
        in_specs=[hb] * 9,
        out_specs=[vm] * (7 + len(sends)),
        scratch_shapes=[
            pltpu.VMEM((width, 2 * LANES), BF16),
            pltpu.SMEM(owner_t.shape, jnp.int32),
            pltpu.SMEM(part_t.shape, jnp.int32),
            pltpu.SemaphoreType.DMA((tok_count // chunk,)),
            pltpu.SemaphoreType.DMA((8,)),
        ],
        compiler_params=pltpu.CompilerParams(vmem_limit_bytes=24 << 20),
        name="kv_project",
        cost_estimate=pl.CostEstimate(
            flops=2 * tok_count * width * 2 * LANES, bytes_accessed=4 * tok_count * width, transcendentals=0
        ),
    )(
        *map(
            distant,
            (owner_t, part_t, tokens, key_weight, value_weight, coarse, fine, query_weight, out_weight),
        )
    )
    kv_rows, bias, *loaded, my_weight = kv_out[:7]
    sent = list(kv_out[7:])

    if direct:
        arrived = {}
        for (pair, g), block in zip(pieces, sent):
            if pair:
                block = lax.ppermute(block, "kv", [(i, i ^ pair) for i in range(devices)])
            arrived[pair, g] = resident(block)
        by_group = [
            [arrived[pair, None if pair in whole else g] for pair in range(devices)]
            for g in range(len(sizes))
        ]
        offsets = [
            [firsts[g] if pair in whole else 0 for pair in range(devices)] for g in range(len(sizes))
        ]
    else:
        got = lax.all_to_all(
            sent[0].reshape((devices, qblocks) + block_shape), "kv", split_axis=0, concat_axis=0, tiled=True
        )
        mine_owner = lax.dynamic_slice_in_dim(owner_t, me * qblocks, qblocks, 1)
        rows = jnp.arange(qblocks, dtype=jnp.int32)
        by_group = [[got[jnp.maximum(mine_owner[slot], 0), rows] for slot in range(chosen)]]
        offsets = [[0] * chosen]

    queries = pl.pallas_call(
        functools.partial(q_kernel, chunk),
        out_shape=pltpu.VMEM((heads, tok_count, LANES), BF16),
        in_specs=[vm] * 4,
        out_specs=vm,
        compiler_params=pltpu.CompilerParams(vmem_limit_bytes=24 << 20),
        name="q_project",
        cost_estimate=pl.CostEstimate(
            flops=2 * tok_count * width * heads * HEAD_DIM,
            bytes_accessed=4 * tok_count * width,
            transcendentals=0,
        ),
    )(*map(resident, (loaded[0], loaded[3], loaded[1], loaded[2])))
    other_weight = resident(lax.ppermute(my_weight, "tp", swap))
    my_weight = resident(my_weight)

    gain = norm_gain.reshape(1, -1)
    cols = norm_gain.shape[0]
    depth = heads * HEAD_DIM
    result = None
    for g, (first, size) in enumerate(zip(firsts, sizes)):
        tokens_here = size * QUERY_BLOCK
        extra = [] if result is None else [result]
        mixed = pl.pallas_call(
            functools.partial(attention_kernel, first, tuple(offsets[g]), PER_DOT),
            out_shape=pltpu.VMEM((tokens_here, depth), BF16),
            in_specs=[vm] * (3 + sources) + [hb] * len(extra),
            out_specs=vm,
            compiler_params=pltpu.CompilerParams(vmem_limit_bytes=24 << 20),
            cost_estimate=pl.CostEstimate(
                flops=4 * tokens_here * heads * LANES * (sources * KEY_BLOCK + QUERY_BLOCK),
                bytes_accessed=tokens_here * depth * 6,
                transcendentals=0,
            ),
        )(resident(queries), resident(kv_rows), resident(bias), *by_group[g], *map(distant, extra))
        other_mixed = resident(lax.ppermute(mixed, "tp", swap))
        own_partial = pl.pallas_call(
            partial_kernel,
            out_shape=pltpu.VMEM((tokens_here, 2 * cols), BF16),
            in_specs=[vm] * 2,
            out_specs=vm,
            compiler_params=pltpu.CompilerParams(vmem_limit_bytes=16 << 20),
            cost_estimate=pl.CostEstimate(
                flops=4 * tokens_here * depth * cols, bytes_accessed=4 * depth * cols, transcendentals=0
            ),
        )(resident(mixed), my_weight)
        result = pl.pallas_call(
            functools.partial(out_kernel, first, OUT_SPLIT),
            out_shape=jax.ShapeDtypeStruct((1, tok_count, cols), BF16),
            in_specs=[vm, vm, vm, vm] + [hb] * len(extra),
            out_specs=hb,
            input_output_aliases={4: 0} if extra else {},
            scratch_shapes=[
                pltpu.VMEM((tokens_here, cols), F32),
                pltpu.VMEM((tokens_here, cols), BF16),
                pltpu.SemaphoreType.DMA((OUT_SPLIT,)),
            ],
            compiler_params=pltpu.CompilerParams(vmem_limit_bytes=16 << 20),
            cost_estimate=pl.CostEstimate(
                flops=4 * tokens_here * depth * cols, bytes_accessed=4 * depth * cols, transcendentals=0
            ),
        )(resident(own_partial), other_mixed, other_weight, gain, *map(distant, extra))
    return result


def solution(mesh):
    placed = (
        P("dp", "kv", None),
        P(None, "tp"),
        P(None, "tp"),
        P(None, "tp"),
        P("tp", None),
        P("tp"),
        P("dp", None, None),
        P("dp", None, None),
    )
    return jax.shard_map(body, mesh=mesh, in_specs=placed, out_specs=P("dp", "kv", "tp"), check_vma=False)
```
